1024 devices in a mesh: fs: 32 (over z, core), tp: 32 (over y, x).
Axes of the slice: x: 4, y: 8, z: 16, core: 2. Of those that a mesh axis runs over, the one named last changes fastest.
Arguments:
- tokens: bfloat16 [4096, 2048], P('fs', 'tp'), may hold values from -6 to 6
- first_gain: float32 [2048], P('fs'), may hold values from 0.1 to 1.9
- first_gate: float32 [2048, 5504], P('fs', 'tp'), may hold values from -0.125 to 0.125
- first_up: float32 [2048, 5504], P('fs', 'tp'), may hold values from -0.125 to 0.125
- first_down: float32 [5504, 2048], P('tp', 'fs'), may hold values from -0.15625 to 0.15625
- first_post: float32 [2048], replicated, may hold values from 0.1 to 1.9
- second_gain: float32 [2048], P('fs'), may hold values from 0.1 to 1.9
- second_gate: float32 [2048, 5504], P('fs', 'tp'), may hold values from -0.125 to 0.125
- second_up: float32 [2048, 5504], P('fs', 'tp'), may hold values from -0.125 to 0.125
- second_down: float32 [5504, 2048], P('tp', 'fs'), may hold values from -0.15625 to 0.15625
- second_post: float32 [2048], replicated, may hold values from 0.1 to 1.9
Outputs:
- mixed: bfloat16 [4096, 2048], P('fs', 'tp')
- gate_one: bfloat16 [2048, 5504], P(None, 'tp')
- up_one: bfloat16 [2048, 5504], P(None, 'tp')
- down_one: bfloat16 [5504, 2048], P('tp')
- gate_two: bfloat16 [2048, 5504], P(None, 'tp')
- up_two: bfloat16 [2048, 5504], P(None, 'tp')
- down_two: bfloat16 [5504, 2048], P('tp')
The draws below stay inside these ranges and needn't reach their ends.
All inputs are finite; a program needn't handle non-finite values.
Results may differ from the reference program's by a relative error of at most 0.015.
Values may be sent and summed in bfloat16 or wider, within the bound.
No kernel may reach another device: no remote copies, remote signals or barrier semaphores. Data moves between devices by JAX's collectives and lax.ppermute only.
A program may use at most 32 MiB of HBM per device.

```python
import jax
import jax.numpy as jnp
from jax import lax

D = 2048
FF = 5504
TOKENS = 4096
N_TP = 32


def spiked(result, own_key, source, target, shards_of, factor):
    def block_of(dim):
        return (jnp.arange(result.shape[dim]) // (result.shape[dim] // shards_of)).reshape((-1,) + (1,) * (result.ndim - 1 - dim))

    near = jax.random.permutation(own_key, shards_of)[block_of(target)]
    far = (block_of(target) + shards_of // 2) % shards_of
    return jnp.where((block_of(source) == near) | (block_of(source) == far), factor * result, result)


def level_of(own_key, shape, shards, least, top_value):
    def one(axis_at, parts):
        draws = jax.random.uniform(jax.random.fold_in(jax.random.fold_in(own_key, 6), axis_at), (parts,), jnp.float32, least / len(shards), top_value / len(shards))
        return jnp.repeat(jnp.exp(draws), shape[axis_at] // parts).reshape((-1,) + (1,) * (len(shape) - axis_at - 1))

    level = one(*shards[0])
    for cut in shards[1:]:
        level = level * one(*cut)
    return level


def centred(own_key, extent, deviation, most, pieces=(), held_as=jnp.bfloat16):
    loudness = level_of(own_key, extent, pieces, -0.22, 0.18) if pieces else 1.0
    entries = jax.random.normal(own_key, extent, jnp.float32) * deviation * loudness
    return jnp.minimum(jnp.maximum(entries, -most), most).astype(held_as)


def bell_draw_with(stream_key, dims, deviation, reach, split, heavy, kind=jnp.bfloat16):
    values = deviation * jax.random.normal(stream_key, dims, jnp.float32)
    if split:
        values = values * level_of(stream_key, dims, split, -0.22, 0.18)
    return jnp.clip(spiked(values, jax.random.fold_in(stream_key, 3), *heavy), -reach, reach).astype(kind)


def setup_inputs(seed: int = 0) -> dict:
    splits = jax.random.split(jax.random.key(seed), 12)
    tokens = centred(splits[0], (TOKENS, D), 1.0, 6.0, ((0, 32), (1, 32)))
    first_gain = jnp.clip(1.0 + 0.18 * jax.random.normal(splits[1], (D,), jnp.float32), 0.1, 1.9)
    first_gate = centred(splits[2], (D, FF), D ** -0.5, 0.125, ((0, 32), (1, 32)), jnp.float32)
    first_up = centred(splits[3], (D, FF), D ** -0.5, 0.125, ((0, 32), (1, 32)), jnp.float32)
    first_down = bell_draw_with(splits[4], (FF, D), FF ** -0.5, 0.15625, ((0, 32), (1, 32)), (0, 1, 32, 2.75), jnp.float32)
    first_post = jnp.clip(1.0 + 0.18 * jax.random.normal(splits[5], (D,), jnp.float32), 0.1, 1.9)
    second_gain = jnp.clip(1.0 + 0.18 * jax.random.normal(splits[6], (D,), jnp.float32), 0.1, 1.9)
    second_gate = centred(splits[7], (D, FF), D ** -0.5, 0.125, ((0, 32), (1, 32)), jnp.float32)
    second_up = centred(splits[8], (D, FF), D ** -0.5, 0.125, ((0, 32), (1, 32)), jnp.float32)
    second_down = bell_draw_with(splits[9], (FF, D), FF ** -0.5, 0.15625, ((0, 32), (1, 32)), (0, 1, 32, 2.75), jnp.float32)
    second_post = jnp.clip(1.0 + 0.18 * jax.random.normal(splits[10], (D,), jnp.float32), 0.1, 1.9)
    return dict(tokens=tokens, first_gain=first_gain, first_gate=first_gate, first_up=first_up, first_down=first_down, first_post=first_post, second_gain=second_gain, second_gate=second_gate, second_up=second_up, second_down=second_down, second_post=second_post)


norm_epsilon = 1e-06

def convert(gain, gate, up, down):
    gate_half = (gain[:, None] * gate).astype(jnp.bfloat16)
    up_half = (gain[:, None] * up).astype(jnp.bfloat16)
    return (gate_half, up_half, down.astype(jnp.bfloat16))

def half_step(rows, gate_w, up_w, down_w, post):
    rows_float = rows.astype(jnp.float32)
    scale = lax.rsqrt(lax.optimization_barrier(jnp.mean(rows_float * rows_float, axis=1, keepdims=True)) + norm_epsilon)
    gate = scale * jnp.dot(rows, gate_w, preferred_element_type=jnp.float32)
    up = scale * jnp.dot(rows, up_w, preferred_element_type=jnp.float32)
    hidden = (jax.nn.silu(gate) * up).astype(jnp.bfloat16)
    block = FF // N_TP

    def add_block(index, total):
        start = (index * block).astype(jnp.int32)
        piece = lax.dynamic_slice_in_dim(hidden, start, block, 1)
        weight = lax.dynamic_slice_in_dim(down_w, start, block, 0)
        part = jnp.dot(piece, weight, preferred_element_type=jnp.float32).astype(jnp.bfloat16)
        part = lax.optimization_barrier(part)
        return total + part.astype(jnp.float32)
    branch = lax.fori_loop(0, N_TP, add_block, jnp.zeros((rows.shape[0], D), jnp.float32))
    post_scale = lax.rsqrt(lax.optimization_barrier(jnp.mean(branch * branch, axis=1, keepdims=True)) + norm_epsilon)
    return (rows_float + 0.5 * branch * post_scale * post[None, :]).astype(jnp.bfloat16)

def reference(tokens, first_gain, first_gate, first_up, first_down, first_post, second_gain, second_gate, second_up, second_down, second_post):
    gate_one, up_one, down_one = convert(first_gain, first_gate, first_up, first_down)
    gate_two, up_two, down_two = convert(second_gain, second_gate, second_up, second_down)
    middle = half_step(tokens, gate_one, up_one, down_one, first_post)
    mixed = half_step(middle, gate_two, up_two, down_two, second_post)
    return (mixed, gate_one, up_one, down_one, gate_two, up_two, down_two)
```

```python
import jax
import jax.numpy as jnp
from jax import lax
from jax.experimental import pallas as pl
from jax.experimental.pallas import tpu as pltpu
from jax.sharding import Mesh
from jax.sharding import PartitionSpec as P


TP = ("tp_0", "tp_1")
FS = ("pair", "parity", "core")


norm_epsilon = 1e-06


def sent_to_all(x, axis):
    peers = lax.axis_size(axis)
    return lax.all_to_all(jnp.broadcast_to(x[None], (peers, *x.shape)), axis, 0, 0, tiled=True)


def gathered_copies(x, axis):
    return sent_to_all(x, axis).reshape(-1, *x.shape[1:])


def sent_and_summed(x, axis):
    peers = lax.axis_size(axis)
    parts = lax.all_to_all(x.reshape(peers, -1, *x.shape[1:]), axis, 0, 0, tiled=True)
    return jnp.sum(parts.astype(jnp.float32), axis=0)


LANE = 128


def aligned(width):
    return -(-width // 16) * 16


def packed_rows(hidden):
    return aligned(-(-3 * aligned(hidden) // 2))


def packed(gain, gate, up, down):
    rows, hidden = gate.shape
    block, half = aligned(hidden), packed_rows(hidden)

    def kernel(gain_ref, gate_ref, up_ref, down_ref, out_ref, tall_ref):
        tall_ref[...] = jnp.zeros_like(tall_ref)
        tall_ref[:hidden, :] = gate_ref[...].T * gain_ref[...]
        tall_ref[block : block + hidden, :] = up_ref[...].T * gain_ref[...]
        tall_ref[2 * block : 2 * block + hidden, :] = down_ref[...].T
        halves = (tall_ref[:half, :], tall_ref[half:, :])
        out_ref[...] = jnp.concatenate(halves, axis=1).astype(jnp.bfloat16)

    return pl.pallas_call(
        kernel,
        out_shape=jax.ShapeDtypeStruct((half, 2 * rows), jnp.bfloat16),
        scratch_shapes=[pltpu.VMEM((2 * half, rows), jnp.float32)],
    )(gain[None, :], gate, up, down.T)


def swapped(own):
    ring = lax.axis_size(FS[:2])
    half = own.shape[0] // 2
    low = lax.ppermute(own[:half], FS[:2], [(i, (i - 1) % ring) for i in range(ring)])
    high = lax.ppermute(own[half:], FS[:2], [(i, (i + 1) % ring) for i in range(ring)])
    return own, low, high


def blocks_of(parity, own, low, high, half):
    pairs = own.shape[0] // (2 * half)
    for at in range(pairs):
        where = low if at < pairs // 2 else high
        for ref, row, slot in ((own, at, parity), (where, at % (pairs // 2), 1 - parity)):
            first = ref[2 * row * half : (2 * row + 1) * half, :]
            second = ref[(2 * row + 1) * half : (2 * row + 2) * half, :]
            side = first.shape[1] // 2
            top = jnp.concatenate((first[:, :side], second[:, :side]), axis=1)
            low_part = jnp.concatenate((first[:, side:], second[:, side:]), axis=1)
            spot = pl.ds(pl.multiple_of((2 * at + slot) * LANE, LANE), LANE)
            yield spot, top, low_part


def mixed_part(parity, slabs, full, hidden):
    features, tokens = full.shape
    block, half = aligned(hidden), packed_rows(hidden)

    def kernel(parity_ref, own_ref, low_ref, high_ref, full_ref, out_ref, down_ref):
        squares = jnp.zeros((1, tokens), jnp.float32)
        total = jnp.zeros((2 * block, tokens), jnp.float32)
        spots = []
        for spot, top, rest in blocks_of(parity_ref[0], own_ref, low_ref, high_ref, half):
            piece = full_ref[spot, :]
            wide = piece.astype(jnp.float32)
            squares += jnp.sum(wide * wide, axis=0, keepdims=True)
            total += jnp.dot(
                jnp.concatenate((top, rest[: 2 * block - half]), axis=0),
                piece,
                preferred_element_type=jnp.float32,
            )
            at = len(spots) * LANE
            down_ref[:, at : at + LANE] = rest[2 * block - half : 3 * block - half]
            spots.append(spot)
        total *= lax.rsqrt(squares / features + norm_epsilon)
        gate = total[:block]
        hidden_value = gate / (1.0 + jnp.exp(-gate)) * total[block:]
        hidden_value = hidden_value.T.astype(jnp.bfloat16)
        for at in range(0, len(spots), 2):
            part = jnp.dot(
                hidden_value,
                down_ref[:, at * LANE : (at + 2) * LANE],
                preferred_element_type=jnp.float32,
            )
            for i in range(2):
                out_ref[spots[at + i], :] = part[:, i * LANE : (i + 1) * LANE].T.astype(jnp.bfloat16)

    vmem = pl.BlockSpec(memory_space=pltpu.VMEM)
    return pl.pallas_call(
        kernel,
        in_specs=[pl.BlockSpec(memory_space=pltpu.SMEM)] + [vmem] * (len(slabs) + 1),
        out_specs=vmem,
        out_shape=jax.ShapeDtypeStruct((features, tokens), jnp.bfloat16),
        scratch_shapes=[pltpu.VMEM((block, features), jnp.bfloat16)],
    )(parity, *slabs, full)


def sampler_slabs(parity, slabs, hidden, features):
    block, half = aligned(hidden), packed_rows(hidden)

    def kernel(parity_ref, own_ref, low_ref, high_ref, gate_ref, up_ref, down_ref):
        split = half - block
        for spot, top, rest in blocks_of(parity_ref[0], own_ref, low_ref, high_ref, half):
            gate_ref[:, spot] = top[:hidden]
            up_ref[:split, spot] = top[block:]
            up_ref[split:, spot] = rest[: hidden - split]
            start = 2 * block - half
            down_ref[:, spot] = rest[start : start + hidden]

    vmem = pl.BlockSpec(memory_space=pltpu.VMEM)
    shape = jax.ShapeDtypeStruct((hidden, features), jnp.bfloat16)
    return pl.pallas_call(
        kernel,
        in_specs=[pl.BlockSpec(memory_space=pltpu.SMEM)] + [vmem] * len(slabs),
        out_specs=[vmem] * 3,
        out_shape=[shape] * 3,
    )(parity, *slabs)


def on_device(
    tokens,
    first_gain,
    first_gate,
    first_up,
    first_down,
    first_post,
    second_gain,
    second_gate,
    second_up,
    second_down,
    second_post,
):
    columns = tokens.shape[1]
    hidden = first_gate.shape[1]
    column_start = lax.axis_index(TP) * columns
    full = gathered_copies(tokens.T, TP)
    parity = lax.axis_index("parity").astype(jnp.int32).reshape(1)
    rows_one = packed(first_gain, first_gate, first_up, first_down)
    own_one = lax.all_gather(rows_one, ("pair", "core"), axis=0, tiled=True)
    rows_two = packed(second_gain, second_gate, second_up, second_down)
    own_two = lax.all_gather(rows_two, ("pair", "core"), axis=0, tiled=True)
    slabs_one = swapped(own_one)
    slabs_two = swapped(own_two)
    features = full.shape[0]
    gate_one, up_one, down_one = sampler_slabs(parity, slabs_one, hidden, features)
    gate_two, up_two, down_two = sampler_slabs(parity, slabs_two, hidden, features)

    partial_value = mixed_part(parity, slabs_one, full, hidden)
    share = lax.optimization_barrier(sent_and_summed(partial_value, TP))
    branch = gathered_copies(share.astype(jnp.bfloat16), TP).astype(jnp.float32)
    scale = lax.rsqrt(jnp.mean(branch * branch, axis=0, keepdims=True) + norm_epsilon)
    middle = (full.astype(jnp.float32) + 0.5 * branch * scale * first_post[:, None]).astype(jnp.bfloat16)

    partial_value = mixed_part(parity, slabs_two, middle, hidden)
    share = sent_and_summed(partial_value, TP)
    squares = sent_to_all(jnp.sum(share * share, axis=0, keepdims=True), TP).sum(axis=0)
    scale = lax.rsqrt(squares / middle.shape[0] + norm_epsilon)
    gain_part = lax.dynamic_slice_in_dim(second_post, column_start, columns, 0)
    own = lax.dynamic_slice_in_dim(middle, column_start, columns, 0)
    mixed = (own.astype(jnp.float32) + 0.5 * share * scale * gain_part[:, None]).astype(jnp.bfloat16)
    return (mixed.T, gate_one.T, up_one.T, down_one, gate_two.T, up_two.T, down_two)


def solution(mesh):
    torus = Mesh(mesh.devices.reshape(-1, 2, 2, 8, 4), (*FS, *TP))
    in_specs = (
        P(FS, TP),
        P(FS),
        P(FS, TP),
        P(FS, TP),
        P(TP, FS),
        P(),
        P(FS),
        P(FS, TP),
        P(FS, TP),
        P(TP, FS),
        P(),
    )
    out_specs = (
        P(FS, TP),
        P(None, TP),
        P(None, TP),
        P(TP, None),
        P(None, TP),
        P(None, TP),
        P(TP, None),
    )

    return jax.shard_map(on_device, mesh=torus, in_specs=in_specs, out_specs=out_specs, check_vma=False)
```

```python
import jax
import jax.numpy as jnp
from jax import lax
from jax.experimental import pallas as pl
from jax.experimental.pallas import tpu as pltpu
from jax.sharding import Mesh
from jax.sharding import PartitionSpec as P


TP = ("tp_0", "tp_1")
FS = ("pair", "parity", "core")


norm_epsilon = 1e-06


def sent_to_all(x, axis):
    peers = lax.axis_size(axis)
    return lax.all_to_all(jnp.broadcast_to(x[None], (peers, *x.shape)), axis, 0, 0, tiled=True)


def gathered_copies(x, axis):
    return sent_to_all(x, axis).reshape(-1, *x.shape[1:])


def sent_and_summed(x, axis):
    peers = lax.axis_size(axis)
    parts = lax.all_to_all(x.reshape(peers, -1, *x.shape[1:]), axis, 0, 0, tiled=True)
    return jnp.sum(parts.astype(jnp.float32), axis=0)


LANE = 128


def aligned(width):
    return -(-width // 16) * 16


def packed_rows(hidden):
    return aligned(-(-3 * aligned(hidden) // 2))


def packed(gain, gate, up, down):
    rows, hidden = gate.shape
    block, half = aligned(hidden), packed_rows(hidden)

    def kernel(gain_ref, gate_ref, up_ref, down_ref, out_ref, tall_ref):
        tall_ref[...] = jnp.zeros_like(tall_ref)
        tall_ref[:hidden, :] = gate_ref[...].T * gain_ref[...]
        tall_ref[block : block + hidden, :] = up_ref[...].T * gain_ref[...]
        tall_ref[2 * block : 2 * block + hidden, :] = down_ref[...].T
        halves = (tall_ref[:half, :], tall_ref[half:, :])
        out_ref[...] = jnp.concatenate(halves, axis=1).astype(jnp.bfloat16)

    return pl.pallas_call(
        kernel,
        out_shape=jax.ShapeDtypeStruct((half, 2 * rows), jnp.bfloat16),
        scratch_shapes=[pltpu.VMEM((2 * half, rows), jnp.float32)],
    )(gain[None, :], gate, up, down.T)


def from_neighbours(own):
    ring = lax.axis_size(FS[:2])
    half = own.shape[0] // 2
    low = lax.ppermute(own[:half], FS[:2], [(i, (i - 1) % ring) for i in range(ring)])
    high = lax.ppermute(own[half:], FS[:2], [(i, (i + 1) % ring) for i in range(ring)])
    return low, high


def from_partner(x):
    return lax.ppermute(x, "core", [(0, 1), (1, 0)])


def blocks_of(place_ref, refs, half):
    parity, core = place_ref[0], place_ref[1]
    alone = len(refs) == 6
    pairs = refs[0].shape[0] // half // (1 if alone else 2)
    for at in range(pairs):
        late = at >= pairs // 2
        row = at % (pairs // 2)
        if alone:
            own, mate, low, high, mate_low, mate_high = refs
            sides = (
                (parity, own, at, mate, at),
                (1 - parity, high if late else low, row, mate_high if late else mate_low, row),
            )
            cores = (core, 1 - core)
        else:
            own, low, high = refs
            other = high if late else low
            sides = (
                (parity, own, 2 * at, own, 2 * at + 1),
                (1 - parity, other, 2 * row, other, 2 * row + 1),
            )
            cores = (0, 1)
        for slot, one, one_row, two, two_row in sides:
            first = one[one_row * half : (one_row + 1) * half, :]
            second = two[two_row * half : (two_row + 1) * half, :]
            yield 2 * at + slot, cores, first, second


def joined(first, second):
    side = first.shape[1] // 2
    top = jnp.concatenate((first[:, :side], second[:, :side]), axis=1)
    rest = jnp.concatenate((first[:, side:], second[:, side:]), axis=1)
    return top, rest


def mixed_part(place, slabs, full, hidden):
    features, tokens = full.shape
    block, half = aligned(hidden), packed_rows(hidden)
    side = LANE // 2

    def kernel(place_ref, *refs):
        *slab_refs, full_ref, out_ref, down_ref = refs
        squares = jnp.zeros((1, tokens), jnp.float32)
        total = jnp.zeros((2 * block, tokens), jnp.float32)
        spots = []
        for spot, cores, first, second in blocks_of(place_ref, slab_refs, half):
            spot = [pl.ds(pl.multiple_of(spot * LANE + core * side, side), side) for core in cores]
            top, rest = joined(first, second)
            piece = jnp.concatenate([full_ref[rows, :] for rows in spot], axis=0)
            wide = piece.astype(jnp.float32)
            squares += jnp.sum(wide * wide, axis=0, keepdims=True)
            total += jnp.dot(
                jnp.concatenate((top, rest[: 2 * block - half]), axis=0),
                piece,
                preferred_element_type=jnp.float32,
            )
            at = len(spots) // 2 * LANE
            down_ref[:, at : at + LANE] = rest[2 * block - half : 3 * block - half]
            spots += spot
        total *= lax.rsqrt(squares / features + norm_epsilon)
        gate = total[:block]
        hidden_value = gate / (1.0 + jnp.exp(-gate)) * total[block:]
        hidden_value = hidden_value.T.astype(jnp.bfloat16)
        for at in range(0, features, 2 * LANE):
            part = jnp.dot(
                hidden_value, down_ref[:, at : at + 2 * LANE], preferred_element_type=jnp.float32
            )
            for i in range(0, 2 * LANE, LANE):
                turned = part[:, i : i + LANE].T.astype(jnp.bfloat16)
                for j in range(2):
                    out_ref[spots[(at + i) // side + j], :] = turned[j * side : (j + 1) * side]

    vmem = pl.BlockSpec(memory_space=pltpu.VMEM)
    return pl.pallas_call(
        kernel,
        in_specs=[pl.BlockSpec(memory_space=pltpu.SMEM)] + [vmem] * (len(slabs) + 1),
        out_specs=vmem,
        out_shape=jax.ShapeDtypeStruct((features, tokens), jnp.bfloat16),
        scratch_shapes=[pltpu.VMEM((block, features), jnp.bfloat16)],
    )(place, *slabs, full)


def sampler_slabs(place, slabs, hidden, features):
    block, half = aligned(hidden), packed_rows(hidden)

    def kernel(place_ref, *refs):
        *slab_refs, gate_ref, up_ref, down_ref = refs
        split = half - block
        for spot, cores, first, second in blocks_of(place_ref, slab_refs, half):
            if len(slab_refs) == 6:
                first, second = (
                    jnp.where(cores[0] == 0, first, second),
                    jnp.where(cores[0] == 0, second, first),
                )
            top, rest = joined(first, second)
            spot = pl.ds(pl.multiple_of(spot * LANE, LANE), LANE)
            gate_ref[:, spot] = top[:hidden]
            up_ref[:split, spot] = top[block:]
            up_ref[split:, spot] = rest[: hidden - split]
            start = 2 * block - half
            down_ref[:, spot] = rest[start : start + hidden]

    vmem = pl.BlockSpec(memory_space=pltpu.VMEM)
    shape = jax.ShapeDtypeStruct((hidden, features), jnp.bfloat16)
    return pl.pallas_call(
        kernel,
        in_specs=[pl.BlockSpec(memory_space=pltpu.SMEM)] + [vmem] * len(slabs),
        out_specs=[vmem] * 3,
        out_shape=[shape] * 3,
    )(place, *slabs)


def on_device(
    tokens,
    first_gain,
    first_gate,
    first_up,
    first_down,
    first_post,
    second_gain,
    second_gate,
    second_up,
    second_down,
    second_post,
):
    columns = tokens.shape[1]
    hidden = first_gate.shape[1]
    column_start = lax.axis_index(TP) * columns
    full = gathered_copies(tokens.T, TP)
    place = jnp.stack([lax.axis_index("parity"), lax.axis_index("core")]).astype(jnp.int32)
    rows_one = packed(first_gain, first_gate, first_up, first_down)
    rows_two = packed(second_gain, second_gate, second_up, second_down)
    own_two = lax.all_gather(rows_two, ("pair", "core"), axis=0, tiled=True)
    own_one = lax.all_gather(rows_one, "pair", axis=0, tiled=True)
    near_one = from_neighbours(own_one)
    mates_one = [from_partner(x) for x in (own_one, *near_one)]
    slabs_one = (own_one, mates_one[0], *near_one, *mates_one[1:])
    slabs_two = (own_two, *from_neighbours(own_two))
    features = full.shape[0]
    gate_one, up_one, down_one = sampler_slabs(place, slabs_one, hidden, features)
    gate_two, up_two, down_two = sampler_slabs(place, slabs_two, hidden, features)

    partial_value = mixed_part(place, slabs_one, full, hidden)
    share = lax.optimization_barrier(sent_and_summed(partial_value, TP))
    branch = gathered_copies(share.astype(jnp.bfloat16), TP).astype(jnp.float32)
    scale = lax.rsqrt(jnp.mean(branch * branch, axis=0, keepdims=True) + norm_epsilon)
    middle = (full.astype(jnp.float32) + 0.5 * branch * scale * first_post[:, None]).astype(jnp.bfloat16)

    partial_value = mixed_part(place, slabs_two, middle, hidden)
    share = sent_and_summed(partial_value, TP)
    squares = sent_to_all(jnp.sum(share * share, axis=0, keepdims=True), TP).sum(axis=0)
    scale = lax.rsqrt(squares / middle.shape[0] + norm_epsilon)
    gain_part = lax.dynamic_slice_in_dim(second_post, column_start, columns, 0)
    own = lax.dynamic_slice_in_dim(middle, column_start, columns, 0).astype(jnp.float32)
    own, moved = lax.optimization_barrier((own, 0.5 * share * gain_part[:, None]))
    mixed = (own + moved * scale).astype(jnp.bfloat16)
    return (mixed.T, gate_one.T, up_one.T, down_one, gate_two.T, up_two.T, down_two)


def solution(mesh):
    torus = Mesh(mesh.devices.reshape(-1, 2, 2, 8, 4), (*FS, *TP))
    in_specs = (
        P(FS, TP),
        P(FS),
        P(FS, TP),
        P(FS, TP),
        P(TP, FS),
        P(),
        P(FS),
        P(FS, TP),
        P(FS, TP),
        P(TP, FS),
        P(),
    )
    out_specs = (
        P(FS, TP),
        P(None, TP),
        P(None, TP),
        P(TP, None),
        P(None, TP),
        P(None, TP),
        P(TP, None),
    )

    return jax.shard_map(on_device, mesh=torus, in_specs=in_specs, out_specs=out_specs, check_vma=False)
```

```python
import jax
import jax.numpy as jnp
from jax import lax
from jax.experimental import pallas as pl
from jax.experimental.pallas import tpu as pltpu
from jax.sharding import Mesh
from jax.sharding import PartitionSpec as P


TP = ("tp_0", "tp_1")
FS = ("pair", "parity", "core")


norm_epsilon = 1e-06


def sent_to_all(x, axis):
    peers = lax.axis_size(axis)
    return lax.all_to_all(jnp.broadcast_to(x[None], (peers, *x.shape)), axis, 0, 0, tiled=True)


def gathered_copies(x, axis):
    return sent_to_all(x, axis).reshape(-1, *x.shape[1:])


def sent_and_summed(x, axis):
    peers = lax.axis_size(axis)
    parts = lax.all_to_all(x.reshape(peers, -1, *x.shape[1:]), axis, 0, 0, tiled=True)
    return jnp.sum(parts.astype(jnp.float32), axis=0)


LANE = 128


def aligned(width):
    return -(-width // 16) * 16


def packed_rows(hidden):
    return aligned(-(-3 * aligned(hidden) // 2))


def packed(*groups):
    rows, hidden = groups[0][1].shape
    block, half = aligned(hidden), packed_rows(hidden)
    count = len(groups)

    def kernel(*refs):
        outs, tall_ref = refs[4 * count : -1], refs[-1]
        tall_ref[...] = jnp.zeros_like(tall_ref)
        for i, out_ref in enumerate(outs):
            gain_ref, gate_ref, up_ref, down_ref = refs[4 * i : 4 * i + 4]
            tall_ref[i, :hidden, :] = gate_ref[...].T * gain_ref[...]
            tall_ref[i, block : block + hidden, :] = up_ref[...].T * gain_ref[...]
            tall_ref[i, 2 * block : 2 * block + hidden, :] = down_ref[...].T
            halves = (tall_ref[i, :half, :], tall_ref[i, half:, :])
            out_ref[...] = jnp.concatenate(halves, axis=1).astype(jnp.bfloat16)

    return pl.pallas_call(
        kernel,
        out_shape=[jax.ShapeDtypeStruct((half, 2 * rows), jnp.bfloat16)] * count,
        scratch_shapes=[pltpu.VMEM((count, 2 * half, rows), jnp.float32)],
    )(*(a for gain, gate, up, down in groups for a in (gain[None, :], gate, up, down.T)))


def from_neighbours(own):
    ring = lax.axis_size(FS[:2])
    half = own.shape[0] // 2
    low = lax.ppermute(own[:half], FS[:2], [(i, (i - 1) % ring) for i in range(ring)])
    high = lax.ppermute(own[half:], FS[:2], [(i, (i + 1) % ring) for i in range(ring)])
    return low, high


def from_partner(x):
    return lax.ppermute(x, "core", [(0, 1), (1, 0)])


def blocks_of(place_ref, refs, half):
    parity, core = place_ref[0], place_ref[1]
    alone = len(refs) == 6
    pairs = refs[0].shape[0] // half // (1 if alone else 2)
    for at in range(pairs):
        late = at >= pairs // 2
        row = at % (pairs // 2)
        if alone:
            own, mate, low, high, mate_low, mate_high = refs
            sides = (
                (parity, own, at, mate, at),
                (1 - parity, high if late else low, row, mate_high if late else mate_low, row),
            )
            cores = (core, 1 - core)
        else:
            own, low, high = refs
            other = high if late else low
            sides = (
                (parity, own, 2 * at, own, 2 * at + 1),
                (1 - parity, other, 2 * row, other, 2 * row + 1),
            )
            cores = (0, 1)
        for slot, one, one_row, two, two_row in sides:
            first = one[one_row * half : (one_row + 1) * half, :]
            second = two[two_row * half : (two_row + 1) * half, :]
            yield 2 * at + slot, cores, first, second


def joined(first, second):
    side = first.shape[1] // 2
    top = jnp.concatenate((first[:, :side], second[:, :side]), axis=1)
    rest = jnp.concatenate((first[:, side:], second[:, side:]), axis=1)
    return top, rest


def mixed_part(place, slabs, full, hidden):
    features, tokens = full.shape
    block, half = aligned(hidden), packed_rows(hidden)
    side = LANE // 2

    def kernel(place_ref, *refs):
        *slab_refs, full_ref, out_ref, down_ref = refs
        squares = jnp.zeros((1, tokens), jnp.float32)
        total = jnp.zeros((2 * block, tokens), jnp.float32)
        spots = []
        for spot, cores, first, second in blocks_of(place_ref, slab_refs, half):
            spot = [pl.ds(pl.multiple_of(spot * LANE + core * side, side), side) for core in cores]
            top, rest = joined(first, second)
            piece = jnp.concatenate([full_ref[rows, :] for rows in spot], axis=0)
            wide = piece.astype(jnp.float32)
            squares += jnp.sum(wide * wide, axis=0, keepdims=True)
            total += jnp.dot(
                jnp.concatenate((top, rest[: 2 * block - half]), axis=0),
                piece,
                preferred_element_type=jnp.float32,
            )
            at = len(spots) // 2 * LANE
            down_ref[:, at : at + LANE] = rest[2 * block - half : 3 * block - half]
            spots += spot
        total *= lax.rsqrt(squares / features + norm_epsilon)
        gate = total[:block]
        hidden_value = gate / (1.0 + jnp.exp(-gate)) * total[block:]
        hidden_value = hidden_value.T.astype(jnp.bfloat16)
        for at in range(0, features, 2 * LANE):
            part = jnp.dot(
                hidden_value, down_ref[:, at : at + 2 * LANE], preferred_element_type=jnp.float32
            )
            for i in range(0, 2 * LANE, LANE):
                turned = part[:, i : i + LANE].T.astype(jnp.bfloat16)
                for j in range(2):
                    out_ref[spots[(at + i) // side + j], :] = turned[j * side : (j + 1) * side]

    vmem = pl.BlockSpec(memory_space=pltpu.VMEM)
    return pl.pallas_call(
        kernel,
        in_specs=[pl.BlockSpec(memory_space=pltpu.SMEM)] + [vmem] * (len(slabs) + 1),
        out_specs=vmem,
        out_shape=jax.ShapeDtypeStruct((features, tokens), jnp.bfloat16),
        scratch_shapes=[pltpu.VMEM((block, features), jnp.bfloat16)],
    )(place, *slabs, full)


def sampler_slabs(place, slabs, hidden, features):
    block, half = aligned(hidden), packed_rows(hidden)

    def kernel(place_ref, *refs):
        *slab_refs, gate_ref, up_ref, down_ref = refs
        split = half - block
        for spot, cores, first, second in blocks_of(place_ref, slab_refs, half):
            if len(slab_refs) == 6:
                first, second = (
                    jnp.where(cores[0] == 0, first, second),
                    jnp.where(cores[0] == 0, second, first),
                )
            top, rest = joined(first, second)
            spot = pl.ds(pl.multiple_of(spot * LANE, LANE), LANE)
            gate_ref[:, spot] = top[:hidden]
            up_ref[:split, spot] = top[block:]
            up_ref[split:, spot] = rest[: hidden - split]
            start = 2 * block - half
            down_ref[:, spot] = rest[start : start + hidden]

    vmem = pl.BlockSpec(memory_space=pltpu.VMEM)
    shape = jax.ShapeDtypeStruct((hidden, features), jnp.bfloat16)
    return pl.pallas_call(
        kernel,
        in_specs=[pl.BlockSpec(memory_space=pltpu.SMEM)] + [vmem] * len(slabs),
        out_specs=[vmem] * 3,
        out_shape=[shape] * 3,
    )(place, *slabs)


def on_device(
    tokens,
    first_gain,
    first_gate,
    first_up,
    first_down,
    first_post,
    second_gain,
    second_gate,
    second_up,
    second_down,
    second_post,
):
    columns = tokens.shape[1]
    hidden = first_gate.shape[1]
    column_start = lax.axis_index(TP) * columns
    full = gathered_copies(tokens.T, TP)
    place = jnp.stack([lax.axis_index("parity"), lax.axis_index("core")]).astype(jnp.int32)
    rows_one, rows_two = packed(
        (first_gain, first_gate, first_up, first_down),
        (second_gain, second_gate, second_up, second_down),
    )
    own_two = lax.all_gather(rows_two, ("pair", "core"), axis=0, tiled=True)
    own_one = lax.all_gather(rows_one, "pair", axis=0, tiled=True)
    near_one = from_neighbours(own_one)
    mates_one = [from_partner(x) for x in (own_one, *near_one)]
    slabs_one = (own_one, mates_one[0], *near_one, *mates_one[1:])
    slabs_two = (own_two, *from_neighbours(own_two))
    features = full.shape[0]
    gate_one, up_one, down_one = sampler_slabs(place, slabs_one, hidden, features)
    gate_two, up_two, down_two = sampler_slabs(place, slabs_two, hidden, features)

    partial_value = mixed_part(place, slabs_one, full, hidden)
    share = lax.optimization_barrier(sent_and_summed(partial_value, TP))
    branch = gathered_copies(share.astype(jnp.bfloat16), TP).astype(jnp.float32)
    scale = lax.rsqrt(jnp.mean(branch * branch, axis=0, keepdims=True) + norm_epsilon)
    middle = (full.astype(jnp.float32) + 0.5 * branch * scale * first_post[:, None]).astype(jnp.bfloat16)

    partial_value = mixed_part(place, slabs_two, middle, hidden)
    share = sent_and_summed(partial_value, TP)
    squares = sent_to_all(jnp.sum(share * share, axis=0, keepdims=True), TP).sum(axis=0)
    scale = lax.rsqrt(squares / middle.shape[0] + norm_epsilon)
    gain_part = lax.dynamic_slice_in_dim(second_post, column_start, columns, 0)
    own = lax.dynamic_slice_in_dim(middle, column_start, columns, 0).astype(jnp.float32)
    own, moved = lax.optimization_barrier((own, 0.5 * share * gain_part[:, None]))
    mixed = (own + moved * scale).astype(jnp.bfloat16)
    return (mixed.T, gate_one.T, up_one.T, down_one, gate_two.T, up_two.T, down_two)


def solution(mesh):
    torus = Mesh(mesh.devices.reshape(-1, 2, 2, 8, 4), (*FS, *TP))
    in_specs = (
        P(FS, TP),
        P(FS),
        P(FS, TP),
        P(FS, TP),
        P(TP, FS),
        P(),
        P(FS),
        P(FS, TP),
        P(FS, TP),
        P(TP, FS),
        P(),
    )
    out_specs = (
        P(FS, TP),
        P(None, TP),
        P(None, TP),
        P(TP, None),
        P(None, TP),
        P(None, TP),
        P(TP, None),
    )

    return jax.shard_map(on_device, mesh=torus, in_specs=in_specs, out_specs=out_specs, check_vma=False)
```

```python
import jax
import jax.numpy as jnp
from jax import lax
from jax.experimental import pallas as pl
from jax.experimental.pallas import tpu as pltpu
from jax.sharding import Mesh
from jax.sharding import PartitionSpec as P


TP = ("tp_0", "tp_1")
FS = ("pair", "parity", "core")


norm_epsilon = 1e-06


def sent_to_all(x, axis):
    peers = lax.axis_size(axis)
    return lax.all_to_all(jnp.broadcast_to(x[None], (peers, *x.shape)), axis, 0, 0, tiled=True)


def gathered_copies(x, axis):
    return sent_to_all(x, axis).reshape(-1, *x.shape[1:])


def sent_and_summed(x, axis):
    peers = lax.axis_size(axis)
    parts = lax.all_to_all(x.reshape(peers, -1, *x.shape[1:]), axis, 0, 0, tiled=True)
    return jnp.sum(parts.astype(jnp.float32), axis=0)


LANE = 128


def aligned(width):
    return -(-width // 16) * 16


def packed_rows(hidden):
    return aligned(-(-3 * aligned(hidden) // 2))


def packed(*groups):
    rows, hidden = groups[0][1].shape
    block, half = aligned(hidden), packed_rows(hidden)
    count = len(groups)

    def kernel(*refs):
        outs, tall_ref = refs[4 * count : -1], refs[-1]
        tall_ref[...] = jnp.zeros_like(tall_ref)
        for i, out_ref in enumerate(outs):
            gain_ref, gate_ref, up_ref, down_ref = refs[4 * i : 4 * i + 4]
            tall_ref[i, :hidden, :] = gate_ref[...].T * gain_ref[...]
            tall_ref[i, block : block + hidden, :] = up_ref[...].T * gain_ref[...]
            tall_ref[i, 2 * block : 2 * block + hidden, :] = down_ref[...].T
            halves = (tall_ref[i, :half, :], tall_ref[i, half:, :])
            out_ref[...] = jnp.concatenate(halves, axis=1).astype(jnp.bfloat16)

    return pl.pallas_call(
        kernel,
        out_shape=[jax.ShapeDtypeStruct((half, 2 * rows), jnp.bfloat16)] * count,
        scratch_shapes=[pltpu.VMEM((count, 2 * half, rows), jnp.float32)],
    )(*(a for gain, gate, up, down in groups for a in (gain[None, :], gate, up, down.T)))


def first_share(pairs, alone):
    return pairs * 5 // 8 if alone else pairs // 2


def from_neighbours(own, alone):
    ring = lax.axis_size(FS[:2])
    pairs = ring // 2
    cut = own.shape[0] // pairs * first_share(pairs, alone)
    low = lax.ppermute(own[:cut], FS[:2], [(i, (i - 1) % ring) for i in range(ring)])
    high = lax.ppermute(own[cut:], FS[:2], [(i, (i + 1) % ring) for i in range(ring)])
    return low, high


def from_partner(x):
    return lax.ppermute(x, "core", [(0, 1), (1, 0)])


def blocks_of(place_ref, refs, half):
    parity, core = place_ref[0], place_ref[1]
    alone = len(refs) == 6
    pairs = refs[0].shape[0] // half // (1 if alone else 2)
    for at in range(pairs):
        share = first_share(pairs, alone)
        late = at >= share
        row = at - share if late else at
        if alone:
            own, mate, low, high, mate_low, mate_high = refs
            sides = (
                (parity, own, at, mate, at),
                (1 - parity, high if late else low, row, mate_high if late else mate_low, row),
            )
            cores = (core, 1 - core)
        else:
            own, low, high = refs
            other = high if late else low
            sides = (
                (parity, own, 2 * at, own, 2 * at + 1),
                (1 - parity, other, 2 * row, other, 2 * row + 1),
            )
            cores = (0, 1)
        for slot, one, one_row, two, two_row in sides:
            first = one[one_row * half : (one_row + 1) * half, :]
            second = two[two_row * half : (two_row + 1) * half, :]
            yield 2 * at + slot, cores, first, second


def joined(first, second):
    side = first.shape[1] // 2
    top = jnp.concatenate((first[:, :side], second[:, :side]), axis=1)
    rest = jnp.concatenate((first[:, side:], second[:, side:]), axis=1)
    return top, rest


def mixed_part(place, slabs, full, hidden):
    features, tokens = full.shape
    block, half = aligned(hidden), packed_rows(hidden)
    side = LANE // 2

    def kernel(place_ref, *refs):
        *slab_refs, full_ref, out_ref, down_ref = refs
        squares = jnp.zeros((1, tokens), jnp.float32)
        total = jnp.zeros((2 * block, tokens), jnp.float32)
        spots = []
        for spot, cores, first, second in blocks_of(place_ref, slab_refs, half):
            spot = [pl.ds(pl.multiple_of(spot * LANE + core * side, side), side) for core in cores]
            top, rest = joined(first, second)
            piece = jnp.concatenate([full_ref[rows, :] for rows in spot], axis=0)
            wide = piece.astype(jnp.float32)
            squares += jnp.sum(wide * wide, axis=0, keepdims=True)
            total += jnp.dot(
                jnp.concatenate((top, rest[: 2 * block - half]), axis=0),
                piece,
                preferred_element_type=jnp.float32,
            )
            at = len(spots) // 2 * LANE
            down_ref[:, at : at + LANE] = rest[2 * block - half : 3 * block - half]
            spots += spot
        total *= lax.rsqrt(squares / features + norm_epsilon)
        gate = total[:block]
        hidden_value = gate / (1.0 + jnp.exp(-gate)) * total[block:]
        hidden_value = hidden_value.T.astype(jnp.bfloat16)
        for at in range(0, features, 2 * LANE):
            part = jnp.dot(
                hidden_value, down_ref[:, at : at + 2 * LANE], preferred_element_type=jnp.float32
            )
            for i in range(0, 2 * LANE, LANE):
                turned = part[:, i : i + LANE].T.astype(jnp.bfloat16)
                for j in range(2):
                    out_ref[spots[(at + i) // side + j], :] = turned[j * side : (j + 1) * side]

    vmem = pl.BlockSpec(memory_space=pltpu.VMEM)
    return pl.pallas_call(
        kernel,
        in_specs=[pl.BlockSpec(memory_space=pltpu.SMEM)] + [vmem] * (len(slabs) + 1),
        out_specs=vmem,
        out_shape=jax.ShapeDtypeStruct((features, tokens), jnp.bfloat16),
        scratch_shapes=[pltpu.VMEM((block, features), jnp.bfloat16)],
    )(place, *slabs, full)


def sampler_slabs(place, slabs, hidden, features):
    block, half = aligned(hidden), packed_rows(hidden)

    def kernel(place_ref, *refs):
        *slab_refs, gate_ref, up_ref, down_ref = refs
        split = half - block
        for spot, cores, first, second in blocks_of(place_ref, slab_refs, half):
            if len(slab_refs) == 6:
                first, second = (
                    jnp.where(cores[0] == 0, first, second),
                    jnp.where(cores[0] == 0, second, first),
                )
            top, rest = joined(first, second)
            spot = pl.ds(pl.multiple_of(spot * LANE, LANE), LANE)
            gate_ref[:, spot] = top[:hidden]
            up_ref[:split, spot] = top[block:]
            up_ref[split:, spot] = rest[: hidden - split]
            start = 2 * block - half
            down_ref[:, spot] = rest[start : start + hidden]

    vmem = pl.BlockSpec(memory_space=pltpu.VMEM)
    shape = jax.ShapeDtypeStruct((hidden, features), jnp.bfloat16)
    return pl.pallas_call(
        kernel,
        in_specs=[pl.BlockSpec(memory_space=pltpu.SMEM)] + [vmem] * len(slabs),
        out_specs=[vmem] * 3,
        out_shape=[shape] * 3,
    )(place, *slabs)


def on_device(
    tokens,
    first_gain,
    first_gate,
    first_up,
    first_down,
    first_post,
    second_gain,
    second_gate,
    second_up,
    second_down,
    second_post,
):
    columns = tokens.shape[1]
    hidden = first_gate.shape[1]
    column_start = lax.axis_index(TP) * columns
    full = gathered_copies(tokens.T, TP)
    place = jnp.stack([lax.axis_index("parity"), lax.axis_index("core")]).astype(jnp.int32)
    rows_one, rows_two = packed(
        (first_gain, first_gate, first_up, first_down),
        (second_gain, second_gate, second_up, second_down),
    )
    own_two = lax.all_gather(rows_two, ("pair", "core"), axis=0, tiled=True)
    own_one = lax.all_gather(rows_one, "pair", axis=0, tiled=True)
    near_one = from_neighbours(own_one, True)
    mates_one = [from_partner(x) for x in (own_one, *near_one)]
    slabs_one = (own_one, mates_one[0], *near_one, *mates_one[1:])
    slabs_two = (own_two, *from_neighbours(own_two, False))
    features = full.shape[0]
    gate_one, up_one, down_one = sampler_slabs(place, slabs_one, hidden, features)
    gate_two, up_two, down_two = sampler_slabs(place, slabs_two, hidden, features)

    partial_value = mixed_part(place, slabs_one, full, hidden)
    share = lax.optimization_barrier(sent_and_summed(partial_value, TP))
    branch = gathered_copies(share.astype(jnp.bfloat16), TP).astype(jnp.float32)
    scale = lax.rsqrt(jnp.mean(branch * branch, axis=0, keepdims=True) + norm_epsilon)
    middle = (full.astype(jnp.float32) + 0.5 * branch * scale * first_post[:, None]).astype(jnp.bfloat16)

    partial_value = mixed_part(place, slabs_two, middle, hidden)
    share = sent_and_summed(partial_value, TP)
    squares = sent_to_all(jnp.sum(share * share, axis=0, keepdims=True), TP).sum(axis=0)
    scale = lax.rsqrt(squares / middle.shape[0] + norm_epsilon)
    gain_part = lax.dynamic_slice_in_dim(second_post, column_start, columns, 0)
    own = lax.dynamic_slice_in_dim(middle, column_start, columns, 0).astype(jnp.float32)
    own, moved = lax.optimization_barrier((own, 0.5 * share * gain_part[:, None]))
    mixed = (own + moved * scale).astype(jnp.bfloat16)
    return (mixed.T, gate_one.T, up_one.T, down_one, gate_two.T, up_two.T, down_two)


def solution(mesh):
    torus = Mesh(mesh.devices.reshape(-1, 2, 2, 8, 4), (*FS, *TP))
    in_specs = (
        P(FS, TP),
        P(FS),
        P(FS, TP),
        P(FS, TP),
        P(TP, FS),
        P(),
        P(FS),
        P(FS, TP),
        P(FS, TP),
        P(TP, FS),
        P(),
    )
    out_specs = (
        P(FS, TP),
        P(None, TP),
        P(None, TP),
        P(TP, None),
        P(None, TP),
        P(None, TP),
        P(TP, None),
    )

    return jax.shard_map(on_device, mesh=torus, in_specs=in_specs, out_specs=out_specs, check_vma=False)
```

```python
import jax
import jax.numpy as jnp
from jax import lax
from jax.experimental import pallas as pl
from jax.experimental.pallas import tpu as pltpu
from jax.sharding import Mesh
from jax.sharding import PartitionSpec as P


TP = ("tp_0", "tp_1")
FS = ("pair", "parity", "core")


norm_epsilon = 1e-06


def sent_to_all(x, axis):
    peers = lax.axis_size(axis)
    return lax.all_to_all(jnp.broadcast_to(x[None], (peers, *x.shape)), axis, 0, 0, tiled=True)


def gathered_copies(x, axis):
    return sent_to_all(x, axis).reshape(-1, *x.shape[1:])


def sent_and_summed(x, axis):
    peers = lax.axis_size(axis)
    parts = lax.all_to_all(x.reshape(peers, -1, *x.shape[1:]), axis, 0, 0, tiled=True)
    return jnp.sum(parts.astype(jnp.float32), axis=0)


LANE = 128


def aligned(width):
    return -(-width // 16) * 16


def packed_rows(hidden):
    return aligned(-(-3 * aligned(hidden) // 2))


def packed(peers, tokens, *groups):
    rows, hidden = groups[0][1].shape
    block, half = aligned(hidden), packed_rows(hidden)
    count = len(groups)

    def kernel(*refs):
        tokens_ref, copies_ref, tall_ref = refs[4 * count], refs[-2], refs[-1]
        outs = refs[4 * count + 1 : -2]
        copies_ref[...] = jnp.broadcast_to(tokens_ref[...][None], copies_ref.shape)
        tall_ref[...] = jnp.zeros_like(tall_ref)
        for i, out_ref in enumerate(outs):
            gain_ref, gate_ref, up_ref, down_ref = refs[4 * i : 4 * i + 4]
            tall_ref[i, :hidden, :] = gate_ref[...].T * gain_ref[...]
            tall_ref[i, block : block + hidden, :] = up_ref[...].T * gain_ref[...]
            tall_ref[i, 2 * block : 2 * block + hidden, :] = down_ref[...].T
            halves = (tall_ref[i, :half, :], tall_ref[i, half:, :])
            out_ref[...] = jnp.concatenate(halves, axis=1).astype(jnp.bfloat16)

    return pl.pallas_call(
        kernel,
        out_shape=[jax.ShapeDtypeStruct((half, 2 * rows), jnp.bfloat16)] * count
        + [jax.ShapeDtypeStruct((peers, *tokens.shape), tokens.dtype)],
        scratch_shapes=[pltpu.VMEM((count, 2 * half, rows), jnp.float32)],
    )(*(a for gain, gate, up, down in groups for a in (gain[None, :], gate, up, down.T)), tokens)


def first_share(pairs, alone):
    return pairs * 5 // 8 if alone else pairs // 2


def from_neighbours(own, alone):
    ring = lax.axis_size(FS[:2])
    pairs = ring // 2
    cut = own.shape[0] // pairs * first_share(pairs, alone)
    low = lax.ppermute(own[:cut], FS[:2], [(i, (i - 1) % ring) for i in range(ring)])
    high = lax.ppermute(own[cut:], FS[:2], [(i, (i + 1) % ring) for i in range(ring)])
    return low, high


def from_partner(x):
    return lax.ppermute(x, "core", [(0, 1), (1, 0)])


def blocks_of(place_ref, refs, half):
    parity, core = place_ref[0], place_ref[1]
    alone = len(refs) == 6
    pairs = refs[0].shape[0] // half // (1 if alone else 2)
    for at in range(pairs):
        share = first_share(pairs, alone)
        late = at >= share
        row = at - share if late else at
        if alone:
            own, mate, low, high, mate_low, mate_high = refs
            sides = (
                (parity, own, at, mate, at),
                (1 - parity, high if late else low, row, mate_high if late else mate_low, row),
            )
            cores = (core, 1 - core)
        else:
            own, low, high = refs
            other = high if late else low
            sides = (
                (parity, own, 2 * at, own, 2 * at + 1),
                (1 - parity, other, 2 * row, other, 2 * row + 1),
            )
            cores = (0, 1)
        for slot, one, one_row, two, two_row in sides:
            first = one[one_row * half : (one_row + 1) * half, :]
            second = two[two_row * half : (two_row + 1) * half, :]
            yield 2 * at + slot, cores, first, second


def joined(first, second):
    side = first.shape[1] // 2
    top = jnp.concatenate((first[:, :side], second[:, :side]), axis=1)
    rest = jnp.concatenate((first[:, side:], second[:, side:]), axis=1)
    return top, rest


def mixed_part(place, slabs, full, hidden):
    features, tokens = full.shape
    block, half = aligned(hidden), packed_rows(hidden)
    side = LANE // 2

    def kernel(place_ref, *refs):
        *slab_refs, full_ref, out_ref, down_ref = refs
        squares = jnp.zeros((1, tokens), jnp.float32)
        total = jnp.zeros((2 * block, tokens), jnp.float32)
        spots = []
        for spot, cores, first, second in blocks_of(place_ref, slab_refs, half):
            spot = [pl.ds(pl.multiple_of(spot * LANE + core * side, side), side) for core in cores]
            top, rest = joined(first, second)
            piece = jnp.concatenate([full_ref[rows, :] for rows in spot], axis=0)
            wide = piece.astype(jnp.float32)
            squares += jnp.sum(wide * wide, axis=0, keepdims=True)
            total += jnp.dot(
                jnp.concatenate((top, rest[: 2 * block - half]), axis=0),
                piece,
                preferred_element_type=jnp.float32,
            )
            at = len(spots) // 2 * LANE
            down_ref[:, at : at + LANE] = rest[2 * block - half : 3 * block - half]
            spots += spot
        total *= lax.rsqrt(squares / features + norm_epsilon)
        gate = total[:block]
        hidden_value = gate / (1.0 + jnp.exp(-gate)) * total[block:]
        hidden_value = hidden_value.T.astype(jnp.bfloat16)
        for at in range(0, features, 2 * LANE):
            part = jnp.dot(
                hidden_value, down_ref[:, at : at + 2 * LANE], preferred_element_type=jnp.float32
            )
            for i in range(0, 2 * LANE, LANE):
                turned = part[:, i : i + LANE].T.astype(jnp.bfloat16)
                for j in range(2):
                    out_ref[spots[(at + i) // side + j], :] = turned[j * side : (j + 1) * side]

    vmem = pl.BlockSpec(memory_space=pltpu.VMEM)
    return pl.pallas_call(
        kernel,
        in_specs=[pl.BlockSpec(memory_space=pltpu.SMEM)] + [vmem] * (len(slabs) + 1),
        out_specs=vmem,
        out_shape=jax.ShapeDtypeStruct((features, tokens), jnp.bfloat16),
        scratch_shapes=[pltpu.VMEM((block, features), jnp.bfloat16)],
    )(place, *slabs, full)


def sampler_slabs(place, slabs, hidden, features):
    block, half = aligned(hidden), packed_rows(hidden)

    def kernel(place_ref, *refs):
        *slab_refs, gate_ref, up_ref, down_ref = refs
        split = half - block
        for spot, cores, first, second in blocks_of(place_ref, slab_refs, half):
            if len(slab_refs) == 6:
                first, second = (
                    jnp.where(cores[0] == 0, first, second),
                    jnp.where(cores[0] == 0, second, first),
                )
            top, rest = joined(first, second)
            spot = pl.ds(pl.multiple_of(spot * LANE, LANE), LANE)
            gate_ref[:, spot] = top[:hidden]
            up_ref[:split, spot] = top[block:]
            up_ref[split:, spot] = rest[: hidden - split]
            start = 2 * block - half
            down_ref[:, spot] = rest[start : start + hidden]

    vmem = pl.BlockSpec(memory_space=pltpu.VMEM)
    shape = jax.ShapeDtypeStruct((hidden, features), jnp.bfloat16)
    return pl.pallas_call(
        kernel,
        in_specs=[pl.BlockSpec(memory_space=pltpu.SMEM)] + [vmem] * len(slabs),
        out_specs=[vmem] * 3,
        out_shape=[shape] * 3,
    )(place, *slabs)


def on_device(
    tokens,
    first_gain,
    first_gate,
    first_up,
    first_down,
    first_post,
    second_gain,
    second_gate,
    second_up,
    second_down,
    second_post,
):
    columns = tokens.shape[1]
    hidden = first_gate.shape[1]
    column_start = lax.axis_index(TP) * columns
    place = jnp.stack([lax.axis_index("parity"), lax.axis_index("core")]).astype(jnp.int32)
    rows_one, rows_two, copies = packed(
        lax.axis_size(TP),
        tokens.T,
        (first_gain, first_gate, first_up, first_down),
        (second_gain, second_gate, second_up, second_down),
    )
    full = lax.all_to_all(copies, TP, 0, 0, tiled=True).reshape(-1, tokens.shape[0])
    own_two = lax.all_gather(rows_two, ("pair", "core"), axis=0, tiled=True)
    own_one = lax.all_gather(rows_one, "pair", axis=0, tiled=True)
    near_one = from_neighbours(own_one, True)
    mates_one = [from_partner(x) for x in (own_one, *near_one)]
    slabs_one = (own_one, mates_one[0], *near_one, *mates_one[1:])
    slabs_two = (own_two, *from_neighbours(own_two, False))
    features = full.shape[0]
    gate_one, up_one, down_one = sampler_slabs(place, slabs_one, hidden, features)
    gate_two, up_two, down_two = sampler_slabs(place, slabs_two, hidden, features)

    partial_value = mixed_part(place, slabs_one, full, hidden)
    share = lax.optimization_barrier(sent_and_summed(partial_value, TP))
    branch = gathered_copies(share.astype(jnp.bfloat16), TP).astype(jnp.float32)
    scale = lax.rsqrt(jnp.mean(branch * branch, axis=0, keepdims=True) + norm_epsilon)
    middle = (full.astype(jnp.float32) + 0.5 * branch * scale * first_post[:, None]).astype(jnp.bfloat16)

    partial_value = mixed_part(place, slabs_two, middle, hidden)
    share = sent_and_summed(partial_value, TP)
    squares = sent_to_all(jnp.sum(share * share, axis=0, keepdims=True), TP).sum(axis=0)
    scale = lax.rsqrt(squares / middle.shape[0] + norm_epsilon)
    gain_part = lax.dynamic_slice_in_dim(second_post, column_start, columns, 0)
    own = lax.dynamic_slice_in_dim(middle, column_start, columns, 0).astype(jnp.float32)
    own, moved = lax.optimization_barrier((own, 0.5 * share * gain_part[:, None]))
    mixed = (own + moved * scale).astype(jnp.bfloat16)
    return (mixed.T, gate_one.T, up_one.T, down_one, gate_two.T, up_two.T, down_two)


def solution(mesh):
    torus = Mesh(mesh.devices.reshape(-1, 2, 2, 8, 4), (*FS, *TP))
    in_specs = (
        P(FS, TP),
        P(FS),
        P(FS, TP),
        P(FS, TP),
        P(TP, FS),
        P(),
        P(FS),
        P(FS, TP),
        P(FS, TP),
        P(TP, FS),
        P(),
    )
    out_specs = (
        P(FS, TP),
        P(None, TP),
        P(None, TP),
        P(TP, None),
        P(None, TP),
        P(None, TP),
        P(TP, None),
    )

    return jax.shard_map(on_device, mesh=torus, in_specs=in_specs, out_specs=out_specs, check_vma=False)
```
